32 devices in a mesh: grp: 2 (over y), fs: 4 (over z), tp: 4 (over x, core).
Axes of the slice: x: 2, y: 2, z: 4, core: 2. Of those that a mesh axis runs over, the one named last changes fastest.
Arguments:
- tokens: bfloat16 [1792, 2048], P(('grp', 'fs'), 'tp'), parts along dimension 0, may hold values from -6 to 6
- route_ids: int32 [1792, 2], P(('grp', 'fs')), parts along dimension 0, may hold values from 0 to 3, all different within a row; in each aligned block of 224 rows (0 to 223, 224 to 447, ...) at most 168 rows name the same one
- route_weights: float32 [1792, 2], P(('grp', 'fs')), parts along dimension 0, may hold values from 0.25 to 1
- norm_gain: float32 [2048], P('fs'), may hold values from 0.1 to 1.9
- gate_master: float32 [4, 2048, 512], P(None, 'fs', 'tp'), may hold values from -0.125 to 0.125
- up_master: float32 [4, 2048, 512], P(None, 'fs', 'tp'), may hold values from -0.125 to 0.125
- down_master: float32 [4, 2048, 512], P(None, 'fs', 'tp'), may hold values from -0.25 to 0.25
Outputs:
- gate_serve: bfloat16 [8, 2048, 512], P(('grp', 'fs'), None, 'tp'), parts along dimension 0
- up_serve: bfloat16 [8, 2048, 512], P(('grp', 'fs'), None, 'tp'), parts along dimension 0
- down_serve: bfloat16 [8, 2048, 512], P(('grp', 'fs'), None, 'tp'), parts along dimension 0
- moe_output: bfloat16 [1792, 2048], P(('grp', 'fs'), 'tp'), parts along dimension 0
The draws below stay inside these ranges and needn't reach their ends.
There are 2 independent parts, one for each index of `grp`. The reference program is written for one: setup_inputs(seed, part) draws one part's arguments, and reference() takes and returns one part's arrays. A program takes and returns all parts, laid end to end along the dimension named above; an argument that names none is the same for every part. Nothing has to cross between parts.
Inputs may be any that keep to these rules, and one draw needn't show every extreme that they name: `route_ids`: the 2 experts of a row differ; within the rows of one index of fs (aligned blocks of 224 rows) no expert is named more than 168 times.
All inputs are finite; a program needn't handle non-finite values.
Results may differ from the reference program's by a relative error of at most 0.012.
Values may be sent and summed in bfloat16 or wider, within the bound.
No kernel may reach another device: no remote copies, remote signals or barrier semaphores. Data moves between devices by JAX's collectives and lax.ppermute only.
A program may use at most 64 MiB of HBM per device.

```python
import math
import jax
import jax.numpy as jnp
import numpy as np
from jax import lax

D = 2048
F = 512
TOP = 2
TOK_DEV = 224
EXPERTS = 4
TOKENS = 896
CAP = 168
N_FS = 4
N_TP = 4


def block_levels(stream_key, extent, split, smallest, top_value):
    def one(dim, shards_of):
        steps = jax.random.uniform(jax.random.fold_in(jax.random.fold_in(stream_key, 6), dim), (shards_of,), jnp.float32, smallest / len(split), top_value / len(split))
        return jnp.repeat(jnp.exp(steps), extent[dim] // shards_of).reshape((-1,) + (1,) * (len(extent) - dim - 1))

    level = one(*split[0])
    for cut in split[1:]:
        level = level * one(*cut)
    return level


def deal_out(stream_key, own, number, rows, number_of, top, bound, lean):
    ranking = jax.random.permutation(stream_key, number_of)
    crowded, ordinary = portions_of(number_of, rows * top, bound, lean, True), portions_of(number_of, rows * top, bound, lean, False)
    places = jnp.arange(number_of)

    def named(sizes, turn):
        used = int((sizes > 0).sum())
        fixed = max(1, used // 4)
        passed = fixed + (places - fixed + turn * (used - fixed)) % max(1, number_of - fixed)
        return jnp.zeros((number_of,), jnp.int32).at[ranking[jnp.where(places < fixed, places, passed)]].set(jnp.asarray(sizes, jnp.int32))

    sizes = jnp.where(number % 4 == 0, named(crowded, number // 4), named(ordinary, number - number // 4 - 1))
    mixed = jax.random.permutation(jax.random.fold_in(own, 3), number_of)
    donor, taker = mixed[0:number_of // 2 * 2:2], mixed[1:number_of // 2 * 2:2]
    margin = jnp.minimum(sizes[donor] - 1, bound - sizes[taker]) // 2
    margin = jnp.where((donor == ranking[0]) | (taker == ranking[0]) | (sizes[taker] == 0), 0, jnp.maximum(margin, 0))
    passed = jax.random.randint(jax.random.fold_in(own, 4), (number_of // 2,), 0, 1 << 20) % (margin + 1)
    sizes = sizes.at[donor].add(-passed).at[taker].add(passed)
    members = jnp.searchsorted(jnp.cumsum(sizes), jnp.arange(rows * top), side="right").astype(jnp.int32)
    listing = members.reshape(top, rows).T
    listing = listing[jax.random.permutation(jax.random.fold_in(own, 1), rows)]
    turn = jax.random.randint(jax.random.fold_in(own, 2), (rows, 1), 0, top)
    return jnp.take_along_axis(listing, (jnp.arange(top)[None, :] + turn) % top, axis=1)


def portions_of(number_of, total, limit, slope, full):
    loads = [(1 << 20) // math.isqrt(rank ** slope) + 1 for rank in range(1, number_of + 1)]
    largest = limit if full else min(limit, max(-(-total // number_of), total * loads[0] // sum(loads)))
    least = 1 if total - largest >= number_of - 1 else 0
    counts, spare = [largest] + [least] * (number_of - 1), total - largest - least * (number_of - 1)
    while spare > 0:
        candidates = [i for i in range(1, number_of) if counts[i] < largest] or [i for i in range(1, number_of) if counts[i] < limit]
        mass, budget = sum([loads[i] for i in candidates]), spare
        for i in candidates:
            more = min(limit - counts[i], max(1, budget * loads[i] // mass), spare)
            counts[i] = counts[i] + more
            spare = spare - more
    return np.array(counts)


def centred(rng, shape, deviation, limit, cuts=(), kind=jnp.bfloat16):
    values = deviation * jax.random.normal(rng, shape, jnp.float32)
    if cuts:
        values = values * block_levels(rng, shape, cuts, -0.22, 0.18)
    return jnp.clip(values, -limit, limit).astype(kind)


def setup_inputs(seed: int = 0, part: int = 0) -> dict:
    key_list = jax.random.split(jax.random.key(seed), 8)
    part_splits = jax.random.split(jax.random.fold_in(key_list[7], part), 8)
    tokens = centred(part_splits[0], (TOKENS, D), 1.0, 6.0, ((0, 4), (1, 4)))
    route_ids_keys = jax.random.split(jax.random.fold_in(part_splits[1], 1), TOKENS // TOK_DEV)
    route_ids_turns = jax.random.permutation(jax.random.fold_in(part_splits[1], 3), TOKENS // TOK_DEV)
    route_ids = jax.vmap(lambda own, number: deal_out(jax.random.fold_in(part_splits[1], 2), own, number, TOK_DEV, EXPERTS, TOP, CAP, 1))(route_ids_keys, route_ids_turns).reshape((TOKENS, TOP))
    route_weights = jnp.clip(0.25 + 0.75 * jax.random.uniform(part_splits[2], (TOKENS, TOP), jnp.float32) ** block_levels(part_splits[2], (TOKENS, TOP), ((0, 4),), -0.2, 0.2), 0.25, 1.0)
    norm_gain = jnp.clip(1.0 + 0.18 * jax.random.normal(key_list[3], (D,), jnp.float32), 0.1, 1.9)
    gate_master = centred(key_list[4], (EXPERTS, D, F), D ** -0.5, 0.125, ((1, 4), (2, 4)), jnp.float32)
    up_master = centred(key_list[5], (EXPERTS, D, F), D ** -0.5, 0.125, ((1, 4), (2, 4)), jnp.float32)
    down_master = centred(key_list[6], (EXPERTS, D, F), F ** -0.5, 0.25, ((1, 4), (2, 4)), jnp.float32)
    return {"tokens": tokens, "route_ids": route_ids, "route_weights": route_weights, "norm_gain": norm_gain, "gate_master": gate_master, "up_master": up_master, "down_master": down_master}


norm_epsilon = 1e-06

def slot_numbers(route_ids, experts, capacity):
    flat_ids = route_ids.reshape(-1)
    onehot = (flat_ids[:, None] == jnp.arange(experts, dtype=jnp.int32)[None, :]).astype(jnp.int32)
    before = jnp.cumsum(onehot, axis=0) - onehot
    position = lax.optimization_barrier(jnp.sum(before * onehot, axis=1))
    return (flat_ids * capacity + position).astype(jnp.int32).reshape(route_ids.shape)

def reference(tokens, route_ids, route_weights, norm_gain, gate_master, up_master, down_master):
    row_gain = norm_gain[None, :, None]
    gate_serve = (gate_master * row_gain).astype(jnp.bfloat16)
    up_serve = (up_master * row_gain).astype(jnp.bfloat16)
    down_serve = down_master.astype(jnp.bfloat16)
    values = tokens.astype(jnp.float32)
    normed = (values * lax.rsqrt(lax.optimization_barrier(jnp.mean(values * values, axis=1, keepdims=True)) + norm_epsilon)).astype(jnp.bfloat16)
    blocks = normed.reshape(N_FS, TOK_DEV, D)
    expert_ids = route_ids.reshape(N_FS, TOK_DEV, TOP).astype(jnp.int32)
    slot_ids = jax.vmap(lambda ids: slot_numbers(ids, EXPERTS, CAP))(expert_ids)
    block_index = jnp.broadcast_to(jnp.arange(N_FS, dtype=jnp.int32)[:, None, None], slot_ids.shape)
    token_rows = jnp.broadcast_to(blocks[:, :, None, :], (N_FS, TOK_DEV, TOP, D))
    buffer = jnp.zeros((N_FS, EXPERTS * CAP, D), jnp.bfloat16).at[block_index, slot_ids].set(token_rows)
    by_expert = jnp.moveaxis(buffer.reshape(N_FS, EXPERTS, CAP, D), 1, 0)

    def expert_out(inputs):
        rows, gate_w, up_w, down_w = inputs
        flat_rows = rows.reshape(N_FS * CAP, D)
        gate_sum = jnp.dot(flat_rows, gate_w, preferred_element_type=jnp.float32)
        up_sum = jnp.dot(flat_rows, up_w, preferred_element_type=jnp.float32)
        hidden = (jax.nn.silu(gate_sum) * up_sum).astype(jnp.bfloat16)
        parts_hidden = hidden.astype(jnp.float32).reshape(N_FS * CAP, N_TP, F // N_TP)
        parts_down = down_w.astype(jnp.float32).reshape(D, N_TP, F // N_TP)
        partial_value = jnp.einsum('rpf,dpf->prd', parts_hidden, parts_down)
        rounded = lax.optimization_barrier(partial_value.astype(jnp.bfloat16)).astype(jnp.float32)
        return lax.optimization_barrier(jnp.sum(rounded, axis=0)).astype(jnp.bfloat16).reshape(N_FS, CAP, D)
    outputs = lax.map(expert_out, (by_expert, gate_serve, up_serve, down_serve))
    position = slot_ids - expert_ids * CAP
    picked = outputs[expert_ids, block_index, position]
    weights = route_weights.reshape(N_FS, TOK_DEV, TOP)[..., None]
    combined = lax.optimization_barrier(jnp.sum(weights * picked.astype(jnp.float32), axis=2))
    return (gate_serve, up_serve, down_serve, combined.reshape(TOKENS, D).astype(jnp.bfloat16))
```

```python
import jax
import jax.numpy as jnp
from jax import lax
from jax.sharding import PartitionSpec as P

norm_epsilon = 1e-06


def slot_numbers(rel_ids, experts, capacity):
    rows = rel_ids.shape[0]
    onehot = rel_ids[:, :, None] == jnp.arange(experts, dtype=jnp.int32)[None, None, :]
    named = jnp.any(onehot, axis=1).astype(jnp.bfloat16)
    earlier = (
        lax.broadcasted_iota(jnp.int32, (rows, rows), 0)
        > lax.broadcasted_iota(jnp.int32, (rows, rows), 1)
    ).astype(jnp.bfloat16)
    before = jnp.dot(earlier, named, preferred_element_type=jnp.float32).astype(jnp.int32)
    position = jnp.sum(before[:, None, :] * onehot.astype(jnp.int32), axis=2)
    return rel_ids * capacity + position


def shift(value, axis, step):
    size = lax.axis_size(axis)
    return lax.ppermute(value, axis, [(i, (i + step) % size) for i in range(size)])


def flip(value, axis, mask):
    return lax.ppermute(value, axis, [(i, i ^ mask) for i in range(lax.axis_size(axis))])


def ring_swap(blocks, axis, sign):
    size = lax.axis_size(axis)
    if size <= 8:
        return [blocks[0]] + [shift(blocks[k], axis, sign * k) for k in range(1, size)]
    me = lax.axis_index(axis)
    stacked = jnp.stack(blocks)
    order = (sign * (jnp.arange(size) - me)) % size
    moved = lax.all_to_all(stacked[order], axis, split_axis=0, concat_axis=0, tiled=True)
    back = (me - sign * jnp.arange(size)) % size
    moved = moved[back]
    return [moved[k] for k in range(size)]


def flip_gather(value, axis):
    size = lax.axis_size(axis)
    held = [value]
    span = size // 2
    got = {0: value}
    while span >= 1:
        for mask in sorted(got):
            got[mask ^ span] = flip(got[mask], axis, span)
        span //= 2
    held = [got[mask] for mask in range(size)]
    return held


def deliver(masters, gain, axis, other):
    size = lax.axis_size(axis)
    me = lax.axis_index(axis)
    experts, rows, columns = masters[0].shape
    per = experts // size

    def cut(first, start, length):
        parts = []
        for master in masters:
            part = lax.dynamic_slice(master, (first, start, 0), (per, length, columns))
            if gain is not None:
                part = part * lax.dynamic_slice(gain, (start,), (length,))[None, :, None]
            parts.append(part.astype(jnp.bfloat16))
        return jnp.stack(parts)

    if size > 8 or lax.axis_size(other) != 2 or rows % 32:
        whole = cut_all(masters, gain)
        return lax.all_to_all(whole, axis, split_axis=1, concat_axis=2, tiled=True)
    side = lax.axis_index(other)
    half = rows // 2
    result = jnp.zeros((len(masters), per, rows * size, columns), jnp.bfloat16)
    pieces = [cut(me * per, 0, rows)]
    for k in range(1, size):
        mine = cut((me + k) % size * per, side * half, half)
        got = shift(mine, axis, k)
        partner = flip(got, other, 1)
        low = jnp.where(side == 0, got, partner)
        high = jnp.where(side == 0, partner, got)
        pieces.append(jnp.concatenate([low, high], axis=2))
    for k in range(size):
        result = lax.dynamic_update_slice(result, pieces[k], (0, 0, (me - k) % size * rows, 0))
    return result


def cut_all(masters, gain):
    parts = []
    for master in masters:
        part = master if gain is None else master * gain[None, :, None]
        parts.append(part.astype(jnp.bfloat16))
    return jnp.stack(parts)


def local(tokens, route_ids, route_weights, norm_gain, gate_master, up_master, down_master):
    experts = gate_master.shape[0]
    shards = lax.axis_size("fs")
    columns = lax.axis_size("tp")
    me = lax.axis_index("fs")
    column = lax.axis_index("tp")
    per = experts // shards
    tok_rows, top_count = route_ids.shape
    width = tokens.shape[1]
    model_width = width * columns
    hidden_width = gate_master.shape[2]
    capacity = max(2, 3 * tok_rows * top_count // (2 * experts))
    rows = shards * capacity

    gate_up = deliver([gate_master, up_master], norm_gain, "fs", "grp")

    rel_ids = (route_ids - me * per) % experts
    slot_ids = slot_numbers(rel_ids, experts, capacity)
    slot_range = jnp.arange(experts * capacity, dtype=jnp.int32)
    selects = [
        (slot_ids[:, k, None] == slot_range[None, :]).astype(jnp.bfloat16)
        for k in range(top_count)
    ]
    placing = selects[0]
    for extra in selects[1:]:
        placing = placing + extra
    buffer = jnp.einsum("ts,td->sd", placing, tokens, preferred_element_type=jnp.float32).astype(
        jnp.bfloat16
    )
    buffer = buffer.reshape(shards, per, capacity, width)
    arrived = ring_swap([buffer[k] for k in range(shards)], "fs", 1)
    if shards > 8:
        arrived = [jnp.concatenate(arrived, axis=1)]
    gathered = [flip_gather(block, "tp") for block in arrived]

    down = deliver([down_master], None, "fs", "grp")[0]
    down_blocks = down.reshape(per, columns, width, hidden_width)
    down_parts = [
        lax.dynamic_index_in_dim(down_blocks, column ^ j, axis=1, keepdims=False)
        for j in range(columns)
    ]
    down_parts = [down_parts[0]] + [flip(down_parts[j], "tp", j) for j in range(1, columns)]

    full = jnp.concatenate([jnp.concatenate(parts, axis=2) for parts in gathered], axis=1)
    values = full.astype(jnp.float32)
    inverse = lax.rsqrt(jnp.sum(values * values, axis=2) / model_width + norm_epsilon)[:, :, None]

    blocks = gate_up.reshape(2, per, columns, width, hidden_width)
    turned = jnp.concatenate(
        [lax.dynamic_index_in_dim(blocks, column ^ j, axis=2, keepdims=False) for j in range(columns)],
        axis=2,
    )
    gate_sum = jnp.einsum("xrd,xdf->xrf", full, turned[0], preferred_element_type=jnp.float32)
    up_sum = jnp.einsum("xrd,xdf->xrf", full, turned[1], preferred_element_type=jnp.float32)
    hidden = (jax.nn.silu(gate_sum * inverse) * (up_sum * inverse)).astype(jnp.bfloat16)

    hidden_all = jnp.concatenate(flip_gather(hidden, "tp"), axis=2)
    down_all = jnp.concatenate(down_parts, axis=2)
    outs = jnp.einsum("xrf,xdf->xrd", hidden_all, down_all, preferred_element_type=jnp.float32)
    outs = outs.astype(jnp.bfloat16).reshape(per, shards, capacity, width)
    returned = ring_swap([outs[:, k] for k in range(shards)], "fs", -1)
    returned = jnp.concatenate(returned, axis=0).reshape(experts * capacity, width)
    combined = jnp.zeros((tok_rows, width), jnp.float32)
    for k in range(top_count):
        picked = jnp.einsum(
            "ts,sd->td", selects[k], returned, preferred_element_type=jnp.float32
        )
        combined = combined + route_weights[:, k : k + 1] * picked
    return (gate_up[0], gate_up[1], down, combined.astype(jnp.bfloat16))


def solution(mesh):
    placed = (
        P(("grp", "fs"), "tp"),
        P(("grp", "fs"), None),
        P(("grp", "fs"), None),
        P("fs"),
        P(None, "fs", "tp"),
        P(None, "fs", "tp"),
        P(None, "fs", "tp"),
    )
    return jax.shard_map(
        local,
        mesh=mesh,
        in_specs=placed,
        out_specs=(
            P(("grp", "fs"), None, "tp"),
            P(("grp", "fs"), None, "tp"),
            P(("grp", "fs"), None, "tp"),
            P(("grp", "fs"), "tp"),
        ),
        check_vma=False,
    )
```
